32 devices in a mesh: kv: 8 (over z, y), tp: 4 (over x, core).
Axes of the slice: x: 2, y: 2, z: 4, core: 2. Of those that a mesh axis runs over, the one named last changes fastest.
Arguments:
- tokens: bfloat16 [4096, 2048], P('kv'), may hold values from -18 to 18
- w_query: bfloat16 [2048, 1024], P(None, 'tp'), may hold values from -0.125 to 0.125
- w_key: bfloat16 [2048, 256], P(None, 'tp'), may hold values from -0.125 to 0.125
- w_value: bfloat16 [2048, 256], P(None, 'tp'), may hold values from -18 to 18
- w_out: bfloat16 [1024, 2048], P(None, 'tp'), may hold values from -0.1875 to 0.1875
- out_gain: float32 [1024], replicated, may hold values from 0.1 to 1.9
- chosen: int32 [4, 64, 8], P('tp', 'kv'), may hold values from -1 to 63, as said below
Outputs:
- mixed_out: bfloat16 [4096, 2048], P('kv', 'tp')
The draws below stay inside these ranges and needn't reach their ends.
Inputs may be any that keep to these rules, and one draw needn't show every extreme that they name: chosen[h, b, 0] is b itself; the other entries of a row are distinct key blocks lying wholly before block b, or -1, placed after all named blocks; for each key head h, the query blocks on one index of kv (its 512 positions) name, together, at most one key block of head h held by any other index of kv.
All inputs are finite; a program needn't handle non-finite values.
Results may differ from the reference program's by a relative error of at most 0.024.
Values may be sent and summed in bfloat16 or wider, within the bound.
A program may use at most 64 MiB of HBM per device.

```python
import jax
import jax.numpy as jnp
from jax import lax

D = 2048
HQ = 16
KVH = 4
HD = 64
BLK = 64
SEL = 8
TOK_DEV = 512
TOKENS = 4096
BLOCKS = 64
N_KV = 8


def draw_tokens(key, part):
    return jax.random.truncated_normal(key, -6.0, 6.0, (TOKENS, D), jnp.float32).astype(jnp.bfloat16)


def draw_w_value(key, part):
    column_head = (jnp.arange(KVH * HD, dtype=jnp.int32) // HD).astype(jnp.float32)
    fraction = column_head / (KVH - 1)
    entries = jax.random.truncated_normal(key, -6.0, 6.0, (D, KVH * HD), jnp.float32)
    factor = 3.0 ** fraction
    return (entries * factor[None, :] * D ** (-0.5)).astype(jnp.bfloat16)


def draw_chosen(key, part):
    per_device = TOK_DEV // BLK
    extra = SEL - 1
    rank_total = min(N_KV, per_device * extra)
    key_one, key_two = jax.random.split(key)
    owner_pick = jax.random.randint(key_one, (KVH, N_KV, N_KV), 0, per_device)
    noise = jax.random.randint(key_two, (KVH, N_KV, N_KV), 0, 1024)
    device_ids = jnp.arange(N_KV, dtype=jnp.int32)[:, None]
    owner_ids = jnp.arange(N_KV, dtype=jnp.int32)[None, :]
    below = owner_ids < device_ids
    forced = below & ((owner_ids == device_ids - 1) | (owner_ids == device_ids - N_KV // 2) | (owner_ids == 0))
    ranking = (noise + 2048 * forced.astype(jnp.int32)[None]) * N_KV + (N_KV - 1 - owner_ids)[None]
    ranking = jnp.where(below[None], ranking, -1)
    ignored, order = lax.top_k(ranking, rank_total)
    block_ids = jnp.arange(BLOCKS, dtype=jnp.int32)
    device = block_ids // per_device
    local_index = block_ids % per_device
    slot = jnp.arange(extra, dtype=jnp.int32)[None, :]
    remote_count = jnp.clip(device - local_index * extra, 0, extra)[:, None]
    rank = jnp.minimum(local_index[:, None] * extra + slot, rank_total - 1)
    order_rows = order[:, device, :]
    owner_sel = jnp.take_along_axis(order_rows, jnp.broadcast_to(rank[None], (KVH, BLOCKS, extra)), axis=2)
    head_index = jnp.arange(KVH, dtype=jnp.int32)[:, None, None]
    candidate = owner_pick[head_index, device[None, :, None], owner_sel]
    remote_block = owner_sel * per_device + candidate
    local_slot = slot - remote_count
    local_block = device[:, None] * per_device + local_slot
    fallback = jnp.where((local_slot >= 0) & (local_slot < local_index[:, None]), local_block, -1)
    picked = jnp.where((slot < remote_count)[None], remote_block, fallback[None])
    own_block = jnp.broadcast_to(block_ids[None, :, None], (KVH, BLOCKS, 1))
    return jnp.concatenate([own_block, picked], axis=2).astype(jnp.int32)


def block_scale(key, dims, cuts, least, high):
    def one(dim, parts):
        draws = jax.random.uniform(jax.random.fold_in(jax.random.fold_in(key, 6), dim), (parts,), jnp.float32, least / len(cuts), high / len(cuts))
        return jnp.repeat(jnp.exp(draws), dims[dim] // parts).reshape((-1,) + (1,) * (len(dims) - dim - 1))

    factor_of = one(*cuts[0])
    for cut in cuts[1:]:
        factor_of = factor_of * one(*cut)
    return factor_of


def centred(rng, shape, width, most, shards=(), held_as=jnp.bfloat16):
    loudness = block_scale(rng, shape, shards, -0.22, 0.18) if shards else 1.0
    result = jax.random.normal(rng, shape, jnp.float32) * width * loudness
    return jnp.minimum(jnp.maximum(result, -most), most).astype(held_as)


def setup_inputs(seed: int = 0) -> dict:
    key_list = jax.random.split(jax.random.key(seed), 8)
    return {
        "tokens": draw_tokens(jax.random.fold_in(key_list[7], 71), 0),
        "w_query": centred(key_list[1], (D, HQ * HD), D ** -0.5, 0.125, ((1, 4),)),
        "w_key": centred(key_list[2], (D, KVH * HD), D ** -0.5, 0.125, ((1, 4),)),
        "w_value": draw_w_value(jax.random.fold_in(key_list[7], 71), 0),
        "w_out": centred(key_list[4], (HQ * HD, D), (HQ * HD) ** -0.5, 0.1875, ((1, 4),)),
        "out_gain": jnp.clip(1.0 + 0.18 * jax.random.normal(key_list[5], (HQ * HD,), jnp.float32), 0.1, 1.9),
        "chosen": draw_chosen(jax.random.fold_in(key_list[7], 71), 0),
    }


rope_base = 500000.0
norm_eps = 1e-06

def rotate(vectors, positions):
    half_size = vectors.shape[-1] // 2
    frequency = rope_base ** (-jnp.arange(half_size, dtype=jnp.float32) / half_size)
    angles = positions.astype(jnp.float32)[:, None] * frequency[None, :]
    cosine = jnp.cos(angles)[:, None, :]
    sine_wave = jnp.sin(angles)[:, None, :]
    lower_half = vectors[..., :half_size]
    upper_half = vectors[..., half_size:]
    return jnp.concatenate([lower_half * cosine - upper_half * sine_wave, upper_half * cosine + lower_half * sine_wave], axis=-1)

def reference(tokens, w_query, w_key, w_value, w_out, out_gain, chosen):
    row_total = tokens.shape[0]
    positions = jnp.arange(row_total, dtype=jnp.int32)
    queries = rotate(jnp.dot(tokens, w_query, preferred_element_type=jnp.float32).reshape(row_total, HQ, HD), positions).astype(jnp.bfloat16)
    key_rows = rotate(jnp.dot(tokens, w_key, preferred_element_type=jnp.float32).reshape(row_total, KVH, HD), positions).astype(jnp.bfloat16)
    value_rows = jnp.dot(tokens, w_value, preferred_element_type=jnp.float32).astype(jnp.bfloat16).reshape(row_total, KVH, HD)
    block_total = row_total // BLK
    group_size = HQ // KVH
    key_blocks = key_rows.reshape(block_total, BLK, KVH, HD).transpose(2, 0, 1, 3)
    value_blocks = value_rows.reshape(block_total, BLK, KVH, HD).transpose(2, 0, 1, 3)
    query_blocks = queries.reshape(block_total, BLK, KVH, group_size, HD)
    head_rows = jnp.arange(KVH, dtype=jnp.int32)[:, None]
    offsets = jnp.arange(BLK, dtype=jnp.int32)
    score_scale = HD ** (-0.5)

    def attend(block_index):
        chosen_ids = chosen[:, block_index, :]
        usable = chosen_ids >= 0
        safe_ids = jnp.maximum(chosen_ids, 0)
        key_part = key_blocks[head_rows, safe_ids].astype(jnp.float32)
        value_part = value_blocks[head_rows, safe_ids].astype(jnp.float32)
        query_part = query_blocks[block_index].astype(jnp.float32)
        scores = jnp.einsum('qhgd,hskd->hgqsk', query_part, key_part) * score_scale
        key_pos = chosen_ids[:, :, None] * BLK + offsets
        query_pos = block_index * BLK + offsets
        allowed = usable[:, None, :, None] & (key_pos[:, None, :, :] <= query_pos[None, :, None, None])
        scores = jnp.where(allowed[:, None], scores, -jnp.inf)
        peak_score = lax.optimization_barrier(jnp.max(scores, axis=(3, 4), keepdims=True))
        weights = jnp.exp(scores - peak_score)
        weights = weights / lax.optimization_barrier(jnp.sum(weights, axis=(3, 4), keepdims=True))
        weights = lax.optimization_barrier(weights.astype(jnp.bfloat16)).astype(jnp.float32)
        mixed_out = jnp.einsum('hgqsk,hskd->qhgd', weights, value_part)
        return mixed_out.reshape(BLK, HQ * HD).astype(jnp.bfloat16)
    attended = lax.map(attend, jnp.arange(block_total, dtype=jnp.int32)).reshape(row_total, HQ * HD)
    attn_f32 = attended.astype(jnp.float32)
    squares = lax.optimization_barrier(jnp.sum(attn_f32 * attn_f32, axis=1))
    inverse = lax.rsqrt(squares / (HQ * HD) + norm_eps)
    scaled = (attn_f32 * out_gain[None, :]).astype(jnp.bfloat16)
    product = jnp.dot(scaled, w_out, preferred_element_type=jnp.float32)
    return (inverse[:, None] * product).astype(jnp.bfloat16)
```

```python
import functools
import math

import jax
import jax.numpy as jnp
import numpy as np
from jax import lax
from jax.experimental import pallas as pl
from jax.experimental.pallas import tpu as pltpu
from jax.sharding import PartitionSpec as P

HD = 64
BLK = 64
ROPE_BASE = 500000.0
NORM_EPS = 1e-06
MASKED = -1e30
MESH = pl.DeviceIdType.MESH
F32 = jnp.float32
BF16 = jnp.bfloat16


def angle_tables(count, step):
    half = HD // 2
    lane = np.arange(2 * HD) % half
    frequency = ROPE_BASE ** (-lane.astype(np.float64) / half)
    angles = (np.arange(count, dtype=np.float64) * step)[:, None] * frequency[None, :]
    return np.cos(angles).astype(np.float32), np.sin(angles).astype(np.float32)


def kernel(
    n_kv,
    n_tp,
    tokens_hbm,
    wq_hbm,
    wk_hbm,
    wv_hbm,
    wo_hbm,
    gain_ref,
    chosen_smem,
    chosen_vmem,
    cos_block,
    sin_block,
    cos_row,
    sin_row,
    out_ref,
    tokens,
    wq,
    w_pair,
    wo,
    cos_tab,
    sin_tab,
    ask_out,
    asks,
    kv_local,
    kv_out,
    kv_in,
    k_pool,
    v_pool,
    q_stack,
    gathered,
    acc,
    sq_acc,
    load_sem,
    ask_send,
    ask_recv,
    kv_send,
    kv_recv,
    near_send,
    far_send,
    relay_send,
    g_recv,
):
    me = lax.axis_index("kv")
    tp = lax.axis_index("tp")
    rows = tokens.shape[0]
    blocks = rows // BLK
    sel = chosen_smem.shape[1]
    feat = wq.shape[1]
    heads = feat // HD
    total_feat = wo.shape[0]
    null_id = n_kv + blocks
    parts = 2
    part = rows // parts

    partner = tp + 1 - 2 * lax.rem(tp, 2)
    far = [lax.rem(tp + 2 * k, n_tp) for k in range(1, n_tp // 2)]

    def peer_loop(body):
        if n_kv <= 8:
            for peer in range(n_kv):
                body(peer)
        else:

            @pl.loop(0, n_kv)
            def _(peer):
                body(peer)

    loads = [
        pltpu.make_async_copy(wk_hbm, w_pair.at[pl.ds(0, HD)], load_sem.at[0]),
        pltpu.make_async_copy(wv_hbm, w_pair.at[pl.ds(HD, HD)], load_sem.at[1]),
    ]
    for i in range(parts):
        view = pl.ds(i * part, part)
        loads.append(pltpu.make_async_copy(tokens_hbm.at[view], tokens.at[view], load_sem.at[2 + i]))
    loads.append(pltpu.make_async_copy(wq_hbm, wq, load_sem.at[2 + parts]))
    loads.append(pltpu.make_async_copy(wo_hbm, wo, load_sem.at[3 + parts]))
    for load in loads:
        load.start()

    ask_out[...] = jnp.full(ask_out.shape, -1, jnp.int32)
    ask_out[:, :sel] = chosen_vmem[...]
    asks[...] = jnp.full(asks.shape, -1, jnp.int32)

    barrier = pltpu.get_barrier_semaphore()

    def greet(peer):
        @pl.when(peer != me)
        def _():
            pl.semaphore_signal(barrier, inc=1, device_id=(peer, tp), device_id_type=MESH)

    peer_loop(greet)
    for other in [partner] + far:
        pl.semaphore_signal(barrier, inc=1, device_id=(me, other), device_id_type=MESH)

    pl.semaphore_wait(barrier, n_kv + len(far))

    def ask_copy(source, owner):
        return pltpu.make_async_remote_copy(
            src_ref=ask_out,
            dst_ref=asks.at[source],
            send_sem=ask_send.at[owner],
            recv_sem=ask_recv.at[source],
            device_id=(owner, tp),
            device_id_type=MESH,
        )

    def kv_copy(owner, taker):
        return pltpu.make_async_remote_copy(
            src_ref=kv_out.at[taker],
            dst_ref=kv_in.at[owner],
            send_sem=kv_send.at[taker],
            recv_sem=kv_recv.at[owner],
            device_id=(taker, tp),
            device_id_type=MESH,
        )

    def start_ask(peer):
        @pl.when(peer < me)
        def _():
            ask_copy(me, peer).start()

    peer_loop(start_ask)

    lane = lax.broadcasted_iota(jnp.int32, (BLK, 2 * HD), 1)
    row = lax.broadcasted_iota(jnp.int32, (BLK, 2 * HD), 0)
    low = lane < HD
    first_half = lax.rem(lane, HD) < HD // 2
    sign = jnp.where(first_half, -1.0, 1.0).astype(F32)
    first_row = pl.multiple_of(me * blocks, blocks)
    block_cos = cos_block[pl.ds(first_row, blocks), :]
    block_sin = sin_block[pl.ds(first_row, blocks), :]
    row_cos, row_sin = cos_row[...], sin_row[...]
    for b in range(blocks):
        bc, bs = block_cos[b : b + 1, :], block_sin[b : b + 1, :]
        cos_tab[pl.ds(b * BLK, BLK), :] = bc * row_cos - bs * row_sin
        sin_tab[pl.ds(b * BLK, BLK), :] = (bs * row_cos + bc * row_sin) * sign

    low_f = jnp.where(low, 1.0, 0.0).astype(F32)
    low_b = low_f.astype(BF16)
    high_b = (1.0 - low_f).astype(BF16)
    onehot = jnp.where(lane - HD == row, 1.0, 0.0).astype(F32)
    causal = jnp.where((lane >= HD) & (row > lane - HD), MASKED, 0.0).astype(BF16)
    k_pool[null_id] = jnp.where(low, 0.0, MASKED).astype(BF16)
    v_pool[null_id] = low_b

    def turn(values, c, s):
        width = values.shape[0]
        lanes = lax.broadcasted_iota(jnp.int32, (width, 2 * HD), 1)
        early = lax.rem(lanes, HD) < HD // 2
        swapped = jnp.where(
            early,
            pltpu.roll(values, 2 * HD - HD // 2, 1),
            pltpu.roll(values, HD // 2, 1),
        )
        return values * c + swapped * s

    loads[0].wait()
    loads[1].wait()
    for i in range(parts):
        loads[2 + i].wait()
        pair = lax.dot_general(
            tokens[pl.ds(i * part, part), :],
            w_pair[...],
            (((1,), (1,)), ((), ())),
            preferred_element_type=F32,
        )
        for j in range(part // BLK):
            b = i * (part // BLK) + j
            piece = pair[j * BLK : (j + 1) * BLK, :]
            view = pl.ds(b * BLK, BLK)
            turned = turn(piece, cos_tab[view, :], sin_tab[view, :])
            both = jnp.where(low, turned, piece).astype(BF16)
            kv_local[b] = both
            k_pool[n_kv + b] = both * low_b
            v_pool[n_kv + b] = both * high_b + low_b

    def take_ask(peer):
        @pl.when(peer > me)
        def _():
            ask_copy(peer, me).wait_recv()

    peer_loop(take_ask)

    def fill(peer):
        place = asks[peer] - me * blocks
        inside = (place >= 0) & (place < blocks)
        index = jnp.max(jnp.where(inside, place, 0))
        kv_out[peer] = kv_local[index]

    peer_loop(fill)

    def start_kv(peer):
        @pl.when(peer > me)
        def _():
            kv_copy(me, peer).start()

    peer_loop(start_kv)

    loads[2 + parts].wait()
    q_scale = math.log2(math.e) * HD ** (-0.5)
    for i in range(parts):
        raw = jnp.dot(tokens[pl.ds(i * part, part), :], wq[...], preferred_element_type=F32)
        for j in range(part // BLK):
            b = i * (part // BLK) + j
            view = pl.ds(b * BLK, BLK)
            c, s = cos_tab[view, :] * q_scale, sin_tab[view, :] * q_scale
            for t in range(heads // 2):
                piece = raw[j * BLK : (j + 1) * BLK, t * 2 * HD : (t + 1) * 2 * HD]
                turned = turn(piece, c, s)
                q_stack[b, pl.ds(2 * t * BLK, BLK), :] = jnp.where(low, turned, onehot).astype(BF16)
                q_stack[b, pl.ds((2 * t + 1) * BLK, BLK), :] = jnp.where(
                    low, pltpu.roll(turned, HD, 1), onehot
                ).astype(BF16)

    def take_kv(peer):
        @pl.when(peer < me)
        def _():
            kv_copy(peer, me).wait_recv()
            got = kv_in[peer]
            k_pool[peer] = got * low_b
            v_pool[peer] = got * high_b + low_b

    peer_loop(take_kv)

    def near_copy(c):
        return pltpu.make_async_remote_copy(
            src_ref=gathered.at[tp, c],
            dst_ref=gathered.at[tp, c],
            send_sem=near_send.at[c],
            recv_sem=g_recv.at[tp, c],
            device_id=(me, partner),
            device_id_type=MESH,
        )

    def far_copy(k, c):
        return pltpu.make_async_remote_copy(
            src_ref=gathered.at[tp, c],
            dst_ref=gathered.at[tp, c],
            send_sem=far_send.at[k, c],
            recv_sem=g_recv.at[tp, c],
            device_id=(me, far[k]),
            device_id_type=MESH,
        )

    def relay_copy(k, c):
        return pltpu.make_async_remote_copy(
            src_ref=gathered.at[far[k], c],
            dst_ref=gathered.at[far[k], c],
            send_sem=relay_send.at[k, c],
            recv_sem=g_recv.at[far[k], c],
            device_id=(me, partner),
            device_id_type=MESH,
        )

    def recv_wait(source, c):
        pltpu.make_async_remote_copy(
            src_ref=gathered.at[source, c],
            dst_ref=gathered.at[source, c],
            send_sem=near_send.at[c],
            recv_sem=g_recv.at[source, c],
            device_id=(me, partner),
            device_id_type=MESH,
        ).wait_recv()

    def relay(c):
        for k in range(len(far)):
            recv_wait(far[k], c)
            relay_copy(k, c).start()

    lag = 4
    for b in range(blocks):
        ids = []
        for s in range(sel):
            named = chosen_smem[b, s]
            place = named - me * blocks
            ids.append(
                jnp.where(
                    named < 0,
                    null_id,
                    jnp.where(place >= 0, n_kv + place, lax.div(jnp.maximum(named, 0), blocks)),
                )
            )
        keys = [k_pool[n_kv + b] + causal] + [k_pool[i] for i in ids[1:]]
        values = [v_pool[n_kv + b]] + [v_pool[i] for i in ids[1:]]
        scores = lax.dot_general(
            q_stack[b],
            jnp.concatenate(keys, axis=0),
            (((1,), (1,)), ((), ())),
            preferred_element_type=F32,
        )
        peak = jnp.max(scores, axis=1, keepdims=True)
        weights = jnp.exp2(scores - peak).astype(BF16)
        mixed = jnp.dot(weights, jnp.concatenate(values, axis=0), preferred_element_type=F32)
        rolled = pltpu.roll(mixed, HD, 1)
        for t in range(heads // 2):
            even = slice(2 * t * BLK, (2 * t + 1) * BLK)
            odd = slice((2 * t + 1) * BLK, (2 * t + 2) * BLK)
            top = jnp.where(low, rolled[even, :], mixed[odd, :])
            bottom = jnp.where(low, mixed[even, :], rolled[odd, :])
            gathered[tp, b, :, t * 2 * HD : (t + 1) * 2 * HD] = (top / bottom).astype(BF16)
        for k in range(len(far)):
            far_copy(k, b).start()
        near_copy(b).start()
        if b >= lag:
            relay(b - lag)

    loads[3 + parts].wait()

    def add_source(source, first, count, fresh):
        height = count * BLK
        view = pl.ds(first * BLK, height)
        heads_f = gathered[source, pl.ds(first, count)].reshape(height, feat).astype(F32)
        squared = heads_f * heads_f
        folded = squared[:, : 2 * HD]
        for t in range(1, feat // (2 * HD)):
            folded = folded + squared[:, t * 2 * HD : (t + 1) * 2 * HD]
        start = pl.multiple_of(source * feat, 2 * HD)
        scaled = (heads_f * gain_ref[:, pl.ds(start, feat)]).astype(BF16)
        product = jnp.dot(scaled, wo[pl.ds(start, feat), :], preferred_element_type=F32)
        if fresh:
            sq_acc[view, :] = folded
            acc[view, :] = product
        else:
            sq_acc[view, :] += folded
            acc[view, :] += product

    add_source(tp, 0, blocks, True)
    for c in range(max(blocks - lag, 0), blocks - 2):
        relay(c)
    for c in range(blocks):
        recv_wait(partner, c)
    add_source(partner, 0, blocks, False)
    for c in range(max(blocks - 2, 0), blocks):
        relay(c)

    group = 2
    for g in range(blocks // group):
        for k in range(len(far)):
            add_source(far[k], g * group, group, False)
            mate = far[k] + 1 - 2 * lax.rem(far[k], 2)
            for c in range(g * group, (g + 1) * group):
                recv_wait(mate, c)
            add_source(mate, g * group, group, False)
        view = pl.ds(g * group * BLK, group * BLK)
        inverse = lax.rsqrt(
            jnp.sum(sq_acc[view, :], axis=1, keepdims=True) / total_feat + NORM_EPS
        )
        out_ref[view, :] = (acc[view, :] * inverse).astype(BF16)

    def drain(peer):
        @pl.when(peer < me)
        def _():
            ask_copy(me, peer).wait_send()

        @pl.when(peer > me)
        def _():
            kv_copy(me, peer).wait_send()

    peer_loop(drain)
    for c in range(blocks):
        near_copy(c).wait_send()
        for k in range(len(far)):
            far_copy(k, c).wait_send()
            relay_copy(k, c).wait_send()


def per_device(n_kv, n_tp, tokens, w_query, w_key, w_value, w_out, out_gain, chosen):
    rows, width = tokens.shape
    blocks = rows // BLK
    feat = w_query.shape[1]
    out_cols = w_out.shape[1]
    pool = n_kv + blocks + 1
    cos_block, sin_block = angle_tables(n_kv * blocks, BLK)
    cos_row, sin_row = angle_tables(BLK, 1)
    far = max(n_tp // 2 - 1, 1)
    hbm = pl.BlockSpec(memory_space=pl.ANY)
    vmem = pl.BlockSpec(memory_space=pltpu.VMEM)
    smem = pl.BlockSpec(memory_space=pltpu.SMEM)
    picks = chosen.reshape(blocks, chosen.shape[2])
    dma = pltpu.SemaphoreType.DMA
    return pl.pallas_call(
        functools.partial(kernel, n_kv, n_tp),
        out_shape=jax.ShapeDtypeStruct((rows, out_cols), BF16),
        in_specs=[hbm] * 5 + [vmem, smem, vmem] + [vmem] * 4,
        out_specs=vmem,
        scratch_shapes=[
            pltpu.VMEM(tokens.shape, BF16),
            pltpu.VMEM(w_query.shape, BF16),
            pltpu.VMEM((2 * HD, width), BF16),
            pltpu.VMEM(w_out.shape, BF16),
            pltpu.VMEM((rows, 2 * HD), F32),
            pltpu.VMEM((rows, 2 * HD), F32),
            pltpu.VMEM((blocks, 2 * HD), jnp.int32),
            pltpu.VMEM((n_kv, blocks, 2 * HD), jnp.int32),
            pltpu.VMEM((blocks, BLK, 2 * HD), BF16),
            pltpu.VMEM((n_kv, BLK, 2 * HD), BF16),
            pltpu.VMEM((n_kv, BLK, 2 * HD), BF16),
            pltpu.VMEM((pool, BLK, 2 * HD), BF16),
            pltpu.VMEM((pool, BLK, 2 * HD), BF16),
            pltpu.VMEM((blocks, feat // HD * BLK, 2 * HD), BF16),
            pltpu.VMEM((n_tp, blocks, BLK, feat), BF16),
            pltpu.VMEM((rows, out_cols), F32),
            pltpu.VMEM((rows, 2 * HD), F32),
            dma((6,)),
            dma((n_kv,)),
            dma((n_kv,)),
            dma((n_kv,)),
            dma((n_kv,)),
            dma((blocks,)),
            dma((far, blocks)),
            dma((far, blocks)),
            dma((n_tp, blocks)),
        ],
        compiler_params=pltpu.CompilerParams(collective_id=0, has_side_effects=True),
        name="layer",
    )(
        tokens,
        w_query,
        w_key.T,
        w_value.T,
        w_out,
        out_gain.reshape(1, -1),
        picks,
        picks,
        cos_block,
        sin_block,
        cos_row,
        sin_row,
    )


def solution(mesh):
    return jax.shard_map(
        functools.partial(per_device, mesh.shape["kv"], mesh.shape["tp"]),
        mesh=mesh,
        in_specs=(
            P("kv", None),
            P(None, "tp"),
            P(None, "tp"),
            P(None, "tp"),
            P(None, "tp"),
            P(),
            P("tp", "kv", None),
        ),
        out_specs=P("kv", "tp"),
        check_vma=False,
    )
```

```python
import functools
import math

import jax
import jax.numpy as jnp
import numpy as np
from jax import lax
from jax.experimental import pallas as pl
from jax.experimental.pallas import tpu as pltpu
from jax.sharding import PartitionSpec as P

HD = 64
BLK = 64
ROPE_BASE = 500000.0
NORM_EPS = 1e-06
MASKED = -1e30
MESH = pl.DeviceIdType.MESH
F32 = jnp.float32
BF16 = jnp.bfloat16


def angle_tables(count, step):
    half = HD // 2
    lane = np.arange(2 * HD) % half
    frequency = ROPE_BASE ** (-lane.astype(np.float64) / half)
    angles = (np.arange(count, dtype=np.float64) * step)[:, None] * frequency[None, :]
    return np.cos(angles).astype(np.float32), np.sin(angles).astype(np.float32)


def kernel(
    n_kv,
    n_tp,
    tokens_hbm,
    wq_hbm,
    wk_hbm,
    wv_hbm,
    wo_hbm,
    gain_hbm,
    chosen_hbm,
    block_hbm,
    row_hbm,
    out_ref,
    gain_ref,
    chosen_smem,
    chosen_vmem,
    block_tab,
    row_tab,
    tokens,
    wq,
    w_pair,
    wo,
    cos_tab,
    sin_tab,
    ask_out,
    asks,
    kv_local,
    kv_out,
    kv_in,
    k_pool,
    v_pool,
    q_stack,
    gathered,
    acc,
    sq_acc,
    load_sem,
    ask_send,
    ask_recv,
    kv_send,
    kv_recv,
    near_send,
    far_send,
    relay_send,
    g_recv,
):
    me = lax.axis_index("kv")
    tp = lax.axis_index("tp")
    rows = tokens.shape[0]
    blocks = rows // BLK
    sel = chosen_smem.shape[1]
    feat = wq.shape[1]
    heads = feat // HD
    total_feat = wo.shape[0]
    null_id = n_kv + blocks
    parts = 2
    part = rows // parts

    partner = tp + 1 - 2 * lax.rem(tp, 2)
    far = [lax.rem(tp + 2 * k, n_tp) for k in range(1, n_tp // 2)]

    def peer_loop(body):
        if n_kv <= 8:
            for peer in range(n_kv):
                body(peer)
        else:

            @pl.loop(0, n_kv)
            def _(peer):
                body(peer)

    asks[...] = jnp.full(asks.shape, -1, jnp.int32)
    barrier = pltpu.get_barrier_semaphore()

    def greet(peer):
        @pl.when(peer != me)
        def _():
            pl.semaphore_signal(barrier, inc=1, device_id=(peer, tp), device_id_type=MESH)

    peer_loop(greet)
    for other in [partner] + far:
        pl.semaphore_signal(barrier, inc=1, device_id=(me, other), device_id_type=MESH)

    first_block = pl.multiple_of(me * blocks, blocks)
    pairs = [
        (block_hbm.at[:, pl.ds(first_block, blocks)], block_tab),
        (row_hbm, row_tab),
        (chosen_hbm, chosen_vmem),
        (chosen_hbm, chosen_smem),
        (wk_hbm, w_pair.at[pl.ds(0, HD)]),
        (wv_hbm, w_pair.at[pl.ds(HD, HD)]),
    ]
    for i in range(parts):
        view = pl.ds(i * part, part)
        pairs.append((tokens_hbm.at[view], tokens.at[view]))
    pairs += [(wq_hbm, wq), (gain_hbm, gain_ref), (wo_hbm, wo)]
    loads = [
        pltpu.make_async_copy(source, target, load_sem.at[n])
        for n, (source, target) in enumerate(pairs)
    ]
    for load in loads:
        load.start()

    def ask_copy(source, owner):
        return pltpu.make_async_remote_copy(
            src_ref=ask_out,
            dst_ref=asks.at[source],
            send_sem=ask_send.at[owner],
            recv_sem=ask_recv.at[source],
            device_id=(owner, tp),
            device_id_type=MESH,
        )

    def kv_copy(owner, taker):
        return pltpu.make_async_remote_copy(
            src_ref=kv_out.at[taker],
            dst_ref=kv_in.at[owner],
            send_sem=kv_send.at[taker],
            recv_sem=kv_recv.at[owner],
            device_id=(taker, tp),
            device_id_type=MESH,
        )

    lane = lax.broadcasted_iota(jnp.int32, (BLK, 2 * HD), 1)
    row = lax.broadcasted_iota(jnp.int32, (BLK, 2 * HD), 0)
    low = lane < HD
    first_half = lax.rem(lane, HD) < HD // 2
    sign = jnp.where(first_half, -1.0, 1.0).astype(F32)
    loads[0].wait()
    loads[1].wait()
    block_cos, block_sin = block_tab[0], block_tab[1]
    row_cos, row_sin = row_tab[0], row_tab[1]
    for b in range(blocks):
        bc, bs = block_cos[b : b + 1, :], block_sin[b : b + 1, :]
        cos_tab[pl.ds(b * BLK, BLK), :] = bc * row_cos - bs * row_sin
        sin_tab[pl.ds(b * BLK, BLK), :] = (bs * row_cos + bc * row_sin) * sign

    low_f = jnp.where(low, 1.0, 0.0).astype(F32)
    low_b = low_f.astype(BF16)
    high_b = (1.0 - low_f).astype(BF16)
    onehot = jnp.where(lane - HD == row, 1.0, 0.0).astype(F32)
    causal = jnp.where((lane >= HD) & (row > lane - HD), MASKED, 0.0).astype(BF16)
    k_pool[null_id] = jnp.where(low, 0.0, MASKED).astype(BF16)
    v_pool[null_id] = low_b

    def turn(values, c, s):
        width = values.shape[0]
        lanes = lax.broadcasted_iota(jnp.int32, (width, 2 * HD), 1)
        early = lax.rem(lanes, HD) < HD // 2
        swapped = jnp.where(
            early,
            pltpu.roll(values, 2 * HD - HD // 2, 1),
            pltpu.roll(values, HD // 2, 1),
        )
        return values * c + swapped * s

    loads[4].wait()
    loads[5].wait()
    for i in range(parts):
        loads[6 + i].wait()
        pair = lax.dot_general(
            tokens[pl.ds(i * part, part), :],
            w_pair[...],
            (((1,), (1,)), ((), ())),
            preferred_element_type=F32,
        )
        for j in range(part // BLK):
            b = i * (part // BLK) + j
            piece = pair[j * BLK : (j + 1) * BLK, :]
            view = pl.ds(b * BLK, BLK)
            turned = turn(piece, cos_tab[view, :], sin_tab[view, :])
            both = jnp.where(low, turned, piece).astype(BF16)
            kv_local[b] = both
            k_pool[n_kv + b] = both * low_b
            v_pool[n_kv + b] = both * high_b + low_b

    loads[6 + parts].wait()
    q_scale = math.log2(math.e) * HD ** (-0.5)
    for i in range(parts):
        raw = jnp.dot(tokens[pl.ds(i * part, part), :], wq[...], preferred_element_type=F32)
        for j in range(part // BLK):
            b = i * (part // BLK) + j
            view = pl.ds(b * BLK, BLK)
            c, s = cos_tab[view, :] * q_scale, sin_tab[view, :] * q_scale
            for t in range(heads // 2):
                piece = raw[j * BLK : (j + 1) * BLK, t * 2 * HD : (t + 1) * 2 * HD]
                turned = turn(piece, c, s)
                q_stack[b, pl.ds(2 * t * BLK, BLK), :] = jnp.where(low, turned, onehot).astype(BF16)
                q_stack[b, pl.ds((2 * t + 1) * BLK, BLK), :] = jnp.where(
                    low, pltpu.roll(turned, HD, 1), onehot
                ).astype(BF16)

    loads[2].wait()
    loads[3].wait()
    ask_out[...] = jnp.full(ask_out.shape, -1, jnp.int32)
    ask_out[:, :sel] = chosen_vmem[...]
    pl.semaphore_wait(barrier, n_kv + len(far))

    def start_ask(peer):
        @pl.when(peer < me)
        def _():
            ask_copy(me, peer).start()

    peer_loop(start_ask)

    def answer(peer):
        @pl.when(peer > me)
        def _():
            ask_copy(peer, me).wait_recv()
            place = asks[peer] - me * blocks
            inside = (place >= 0) & (place < blocks)
            index = jnp.max(jnp.where(inside, place, 0))
            kv_out[peer] = kv_local[index]
            kv_copy(me, peer).start()

    peer_loop(answer)

    def take_kv(peer):
        @pl.when(peer < me)
        def _():
            kv_copy(peer, me).wait_recv()
            got = kv_in[peer]
            k_pool[peer] = got * low_b
            v_pool[peer] = got * high_b + low_b

    peer_loop(lambda peer: take_kv(n_kv - 1 - peer))

    def near_copy(c):
        return pltpu.make_async_remote_copy(
            src_ref=gathered.at[tp, c],
            dst_ref=gathered.at[tp, c],
            send_sem=near_send.at[c],
            recv_sem=g_recv.at[tp, c],
            device_id=(me, partner),
            device_id_type=MESH,
        )

    def far_copy(k, c):
        return pltpu.make_async_remote_copy(
            src_ref=gathered.at[tp, c],
            dst_ref=gathered.at[tp, c],
            send_sem=far_send.at[k, c],
            recv_sem=g_recv.at[tp, c],
            device_id=(me, far[k]),
            device_id_type=MESH,
        )

    def relay_copy(k, c):
        return pltpu.make_async_remote_copy(
            src_ref=gathered.at[far[k], c],
            dst_ref=gathered.at[far[k], c],
            send_sem=relay_send.at[k, c],
            recv_sem=g_recv.at[far[k], c],
            device_id=(me, partner),
            device_id_type=MESH,
        )

    def recv_wait(source, c):
        pltpu.make_async_remote_copy(
            src_ref=gathered.at[source, c],
            dst_ref=gathered.at[source, c],
            send_sem=near_send.at[c],
            recv_sem=g_recv.at[source, c],
            device_id=(me, partner),
            device_id_type=MESH,
        ).wait_recv()

    def relay(c):
        for k in range(len(far)):
            recv_wait(far[k], c)
            relay_copy(k, c).start()

    for b in range(blocks):
        ids = []
        for s in range(sel):
            named = chosen_smem[b, s]
            place = named - me * blocks
            ids.append(
                jnp.where(
                    named < 0,
                    null_id,
                    jnp.where(place >= 0, n_kv + place, lax.div(jnp.maximum(named, 0), blocks)),
                )
            )
        keys = [k_pool[n_kv + b] + causal] + [k_pool[i] for i in ids[1:]]
        values = [v_pool[n_kv + b]] + [v_pool[i] for i in ids[1:]]
        scores = lax.dot_general(
            q_stack[b],
            jnp.concatenate(keys, axis=0),
            (((1,), (1,)), ((), ())),
            preferred_element_type=F32,
        )
        peak = jnp.max(scores, axis=1, keepdims=True)
        weights = jnp.exp2(scores - peak).astype(BF16)
        mixed = jnp.dot(weights, jnp.concatenate(values, axis=0), preferred_element_type=F32)
        rolled = pltpu.roll(mixed, HD, 1)
        for t in range(heads // 2):
            even = slice(2 * t * BLK, (2 * t + 1) * BLK)
            odd = slice((2 * t + 1) * BLK, (2 * t + 2) * BLK)
            top = jnp.where(low, rolled[even, :], mixed[odd, :])
            bottom = jnp.where(low, mixed[even, :], rolled[odd, :])
            gathered[tp, b, :, t * 2 * HD : (t + 1) * 2 * HD] = (top / bottom).astype(BF16)
        for k in range(len(far)):
            far_copy(k, b).start()
        near_copy(b).start()

    loads[7 + parts].wait()
    loads[8 + parts].wait()

    def add_source(source, first, count, fresh):
        height = count * BLK
        view = pl.ds(first * BLK, height)
        heads_f = gathered[source, pl.ds(first, count)].reshape(height, feat).astype(F32)
        squared = heads_f * heads_f
        folded = squared[:, : 2 * HD]
        for t in range(1, feat // (2 * HD)):
            folded = folded + squared[:, t * 2 * HD : (t + 1) * 2 * HD]
        start = pl.multiple_of(source * feat, 2 * HD)
        scaled = (heads_f * gain_ref[:, pl.ds(start, feat)]).astype(BF16)
        product = jnp.dot(scaled, wo[pl.ds(start, feat), :], preferred_element_type=F32)
        if fresh:
            sq_acc[view, :] = folded
            acc[view, :] = product
        else:
            sq_acc[view, :] += folded
            acc[view, :] += product

    def finish(c):
        view = pl.ds(c * BLK, BLK)
        recv_wait(partner, c)
        add_source(partner, c, 1, False)
        for k in range(len(far)):
            mate = far[k] + 1 - 2 * lax.rem(far[k], 2)
            recv_wait(mate, c)
            add_source(mate, c, 1, False)
        inverse = lax.rsqrt(
            jnp.sum(sq_acc[view, :], axis=1, keepdims=True) / total_feat + NORM_EPS
        )
        out_ref[view, :] = (acc[view, :] * inverse).astype(BF16)

    add_source(tp, 0, blocks, True)
    lag = 2
    for c in range(blocks + lag):
        if c < blocks:
            relay(c)
            for k in range(len(far)):
                add_source(far[k], c, 1, False)
        if c >= lag:
            finish(c - lag)

    def drain(peer):
        @pl.when(peer < me)
        def _():
            ask_copy(me, peer).wait_send()

        @pl.when(peer > me)
        def _():
            kv_copy(me, peer).wait_send()

    peer_loop(drain)
    for c in range(blocks):
        near_copy(c).wait_send()
        for k in range(len(far)):
            far_copy(k, c).wait_send()
            relay_copy(k, c).wait_send()


def per_device(n_kv, n_tp, tokens, w_query, w_key, w_value, w_out, out_gain, chosen):
    rows, width = tokens.shape
    blocks = rows // BLK
    feat = w_query.shape[1]
    out_cols = w_out.shape[1]
    pool = n_kv + blocks + 1
    block_table = np.stack(angle_tables(n_kv * blocks, BLK))
    row_table = np.stack(angle_tables(BLK, 1))
    far = max(n_tp // 2 - 1, 1)
    hbm = pl.BlockSpec(memory_space=pl.ANY)
    vmem = pl.BlockSpec(memory_space=pltpu.VMEM)
    picks = chosen.reshape(blocks, chosen.shape[2])
    dma = pltpu.SemaphoreType.DMA
    return pl.pallas_call(
        functools.partial(kernel, n_kv, n_tp),
        out_shape=pltpu.VMEM((rows, out_cols), BF16),
        in_specs=[hbm] * 9,
        out_specs=vmem,
        scratch_shapes=[
            pltpu.VMEM((1, out_gain.shape[0]), F32),
            pltpu.SMEM(picks.shape, jnp.int32),
            pltpu.VMEM(picks.shape, jnp.int32),
            pltpu.VMEM((2, blocks, 2 * HD), F32),
            pltpu.VMEM((2, BLK, 2 * HD), F32),
            pltpu.VMEM(tokens.shape, BF16),
            pltpu.VMEM(w_query.shape, BF16),
            pltpu.VMEM((2 * HD, width), BF16),
            pltpu.VMEM(w_out.shape, BF16),
            pltpu.VMEM((rows, 2 * HD), F32),
            pltpu.VMEM((rows, 2 * HD), F32),
            pltpu.VMEM((blocks, 2 * HD), jnp.int32),
            pltpu.VMEM((n_kv, blocks, 2 * HD), jnp.int32),
            pltpu.VMEM((blocks, BLK, 2 * HD), BF16),
            pltpu.VMEM((n_kv, BLK, 2 * HD), BF16),
            pltpu.VMEM((n_kv, BLK, 2 * HD), BF16),
            pltpu.VMEM((pool, BLK, 2 * HD), BF16),
            pltpu.VMEM((pool, BLK, 2 * HD), BF16),
            pltpu.VMEM((blocks, feat // HD * BLK, 2 * HD), BF16),
            pltpu.VMEM((n_tp, blocks, BLK, feat), BF16),
            pltpu.VMEM((rows, out_cols), F32),
            pltpu.VMEM((rows, 2 * HD), F32),
            dma((11,)),
            dma((n_kv,)),
            dma((n_kv,)),
            dma((n_kv,)),
            dma((n_kv,)),
            dma((blocks,)),
            dma((far, blocks)),
            dma((far, blocks)),
            dma((n_tp, blocks)),
        ],
        compiler_params=pltpu.CompilerParams(collective_id=0, has_side_effects=True),
        name="layer",
    )(
        tokens,
        w_query,
        w_key.T,
        w_value.T,
        w_out,
        out_gain.reshape(1, -1),
        picks,
        block_table,
        row_table,
    )


def solution(mesh):
    return jax.shard_map(
        functools.partial(per_device, mesh.shape["kv"], mesh.shape["tp"]),
        mesh=mesh,
        in_specs=(
            P("kv", None),
            P(None, "tp"),
            P(None, "tp"),
            P(None, "tp"),
            P(None, "tp"),
            P(),
            P("tp", "kv", None),
        ),
        out_specs=P("kv", "tp"),
        check_vma=False,
    )
```

```python
import functools
import math

import jax
import jax.numpy as jnp
import numpy as np
from jax import lax
from jax.experimental import pallas as pl
from jax.experimental.pallas import tpu as pltpu
from jax.sharding import PartitionSpec as P

HD = 64
BLK = 64
ROPE_BASE = 500000.0
NORM_EPS = 1e-06
MASKED = -1e30
GROUP = 2
MESH = pl.DeviceIdType.MESH
F32 = jnp.float32
BF16 = jnp.bfloat16


def angle_tables(count, step):
    half = HD // 2
    lane = np.arange(2 * HD) % half
    frequency = ROPE_BASE ** (-lane.astype(np.float64) / half)
    angles = (np.arange(count, dtype=np.float64) * step)[:, None] * frequency[None, :]
    return np.cos(angles).astype(np.float32), np.sin(angles).astype(np.float32)


def kernel(
    n_kv,
    n_tp,
    tokens_hbm,
    wq_hbm,
    wk_hbm,
    wv_hbm,
    wo_hbm,
    gain_hbm,
    chosen_hbm,
    block_hbm,
    row_hbm,
    out_ref,
    gain_ref,
    chosen_smem,
    chosen_vmem,
    block_tab,
    row_tab,
    tokens,
    wq,
    w_pair,
    wo,
    cos_tab,
    sin_tab,
    ask_out,
    asks,
    kv_local,
    kv_out,
    kv_in,
    k_pool,
    v_pool,
    q_stack,
    gathered,
    acc,
    sq_acc,
    load_sem,
    ask_send,
    ask_recv,
    kv_send,
    kv_recv,
    near_send,
    far_send,
    relay_send,
    g_recv,
):
    me = lax.axis_index("kv")
    tp = lax.axis_index("tp")
    rows = tokens.shape[0]
    blocks = rows // BLK
    sel = chosen_smem.shape[1]
    feat = wq.shape[1]
    heads = feat // HD
    total_feat = wo.shape[0]
    null_id = n_kv + blocks
    parts = 2
    part = rows // parts

    partner = tp + 1 - 2 * lax.rem(tp, 2)
    far = [lax.rem(tp + 2 * k, n_tp) for k in range(1, n_tp // 2)]

    def peer_loop(body):
        if n_kv <= 8:
            for peer in range(n_kv):
                body(peer)
        else:

            @pl.loop(0, n_kv)
            def _(peer):
                body(peer)

    asks[...] = jnp.full(asks.shape, -1, jnp.int32)
    barrier = pltpu.get_barrier_semaphore()

    def greet(peer):
        @pl.when(peer != me)
        def _():
            pl.semaphore_signal(barrier, inc=1, device_id=(peer, tp), device_id_type=MESH)

    peer_loop(greet)
    for other in [partner] + far:
        pl.semaphore_signal(barrier, inc=1, device_id=(me, other), device_id_type=MESH)

    first_block = pl.multiple_of(me * blocks, blocks)
    pairs = [
        (block_hbm.at[:, pl.ds(first_block, blocks)], block_tab),
        (row_hbm, row_tab),
        (chosen_hbm, chosen_vmem),
        (chosen_hbm, chosen_smem),
        (wk_hbm, w_pair.at[pl.ds(0, HD)]),
        (wv_hbm, w_pair.at[pl.ds(HD, HD)]),
    ]
    for i in range(parts):
        view = pl.ds(i * part, part)
        pairs.append((tokens_hbm.at[view], tokens.at[view]))
    pairs += [(wq_hbm, wq), (gain_hbm, gain_ref), (wo_hbm, wo)]
    loads = [
        pltpu.make_async_copy(source, target, load_sem.at[n])
        for n, (source, target) in enumerate(pairs)
    ]
    for load in loads:
        load.start()

    def ask_copy(source, owner):
        return pltpu.make_async_remote_copy(
            src_ref=ask_out,
            dst_ref=asks.at[source],
            send_sem=ask_send.at[owner],
            recv_sem=ask_recv.at[source],
            device_id=(owner, tp),
            device_id_type=MESH,
        )

    def kv_copy(owner, taker):
        return pltpu.make_async_remote_copy(
            src_ref=kv_out.at[taker],
            dst_ref=kv_in.at[owner],
            send_sem=kv_send.at[taker],
            recv_sem=kv_recv.at[owner],
            device_id=(taker, tp),
            device_id_type=MESH,
        )

    lane = lax.broadcasted_iota(jnp.int32, (BLK, 2 * HD), 1)
    row = lax.broadcasted_iota(jnp.int32, (BLK, 2 * HD), 0)
    low = lane < HD
    first_half = lax.rem(lane, HD) < HD // 2
    sign = jnp.where(first_half, -1.0, 1.0).astype(F32)
    loads[0].wait()
    loads[1].wait()
    block_cos, block_sin = block_tab[0], block_tab[1]
    row_cos, row_sin = row_tab[0], row_tab[1]
    for b in range(blocks):
        bc, bs = block_cos[b : b + 1, :], block_sin[b : b + 1, :]
        cos_tab[pl.ds(b * BLK, BLK), :] = bc * row_cos - bs * row_sin
        sin_tab[pl.ds(b * BLK, BLK), :] = (bs * row_cos + bc * row_sin) * sign

    low_f = jnp.where(low, 1.0, 0.0).astype(F32)
    low_b = low_f.astype(BF16)
    high_b = (1.0 - low_f).astype(BF16)
    onehot = jnp.where(lane - HD == row, 1.0, 0.0).astype(F32)
    causal = jnp.where((lane >= HD) & (row > lane - HD), MASKED, 0.0).astype(BF16)
    k_pool[null_id] = jnp.where(low, 0.0, MASKED).astype(BF16)
    v_pool[null_id] = low_b

    def turn(values, c, s):
        width = values.shape[0]
        lanes = lax.broadcasted_iota(jnp.int32, (width, 2 * HD), 1)
        early = lax.rem(lanes, HD) < HD // 2
        swapped = jnp.where(
            early,
            pltpu.roll(values, 2 * HD - HD // 2, 1),
            pltpu.roll(values, HD // 2, 1),
        )
        return values * c + swapped * s

    loads[4].wait()
    loads[5].wait()
    for i in range(parts):
        loads[6 + i].wait()
        pair = lax.dot_general(
            tokens[pl.ds(i * part, part), :],
            w_pair[...],
            (((1,), (1,)), ((), ())),
            preferred_element_type=F32,
        )
        for j in range(part // BLK):
            b = i * (part // BLK) + j
            piece = pair[j * BLK : (j + 1) * BLK, :]
            view = pl.ds(b * BLK, BLK)
            turned = turn(piece, cos_tab[view, :], sin_tab[view, :])
            both = jnp.where(low, turned, piece).astype(BF16)
            kv_local[b] = both
            k_pool[n_kv + b] = both * low_b
            v_pool[n_kv + b] = both * high_b + low_b

    loads[6 + parts].wait()
    q_scale = math.log2(math.e) * HD ** (-0.5)
    for i in range(parts):
        raw = jnp.dot(tokens[pl.ds(i * part, part), :], wq[...], preferred_element_type=F32)
        for j in range(part // BLK):
            b = i * (part // BLK) + j
            view = pl.ds(b * BLK, BLK)
            c, s = cos_tab[view, :] * q_scale, sin_tab[view, :] * q_scale
            for t in range(heads // 2):
                piece = raw[j * BLK : (j + 1) * BLK, t * 2 * HD : (t + 1) * 2 * HD]
                turned = turn(piece, c, s)
                q_stack[b, pl.ds(2 * t * BLK, BLK), :] = jnp.where(low, turned, onehot).astype(BF16)
                q_stack[b, pl.ds((2 * t + 1) * BLK, BLK), :] = jnp.where(
                    low, pltpu.roll(turned, HD, 1), onehot
                ).astype(BF16)

    loads[2].wait()
    loads[3].wait()
    ask_out[...] = jnp.full(ask_out.shape, -1, jnp.int32)
    ask_out[:, :sel] = chosen_vmem[...]
    pl.semaphore_wait(barrier, n_kv + len(far))

    def start_ask(peer):
        @pl.when(peer < me)
        def _():
            ask_copy(me, peer).start()

    peer_loop(start_ask)

    def answer(peer):
        @pl.when(peer > me)
        def _():
            ask_copy(peer, me).wait_recv()
            place = asks[peer] - me * blocks
            inside = (place >= 0) & (place < blocks)
            index = jnp.max(jnp.where(inside, place, 0))
            kv_out[peer] = kv_local[index]
            kv_copy(me, peer).start()

    peer_loop(answer)

    def take_kv(peer):
        @pl.when(peer < me)
        def _():
            kv_copy(peer, me).wait_recv()
            got = kv_in[peer]
            k_pool[peer] = got * low_b
            v_pool[peer] = got * high_b + low_b

    peer_loop(lambda peer: take_kv(n_kv - 1 - peer))

    group = math.gcd(GROUP, blocks)
    chunks = blocks // group

    def near_copy(c):
        return pltpu.make_async_remote_copy(
            src_ref=gathered.at[tp, pl.ds(c * group, group)],
            dst_ref=gathered.at[tp, pl.ds(c * group, group)],
            send_sem=near_send.at[c],
            recv_sem=g_recv.at[tp, c],
            device_id=(me, partner),
            device_id_type=MESH,
        )

    def far_copy(k, c):
        return pltpu.make_async_remote_copy(
            src_ref=gathered.at[tp, pl.ds(c * group, group)],
            dst_ref=gathered.at[tp, pl.ds(c * group, group)],
            send_sem=far_send.at[k, c],
            recv_sem=g_recv.at[tp, c],
            device_id=(me, far[k]),
            device_id_type=MESH,
        )

    def relay_copy(k, c):
        return pltpu.make_async_remote_copy(
            src_ref=gathered.at[far[k], pl.ds(c * group, group)],
            dst_ref=gathered.at[far[k], pl.ds(c * group, group)],
            send_sem=relay_send.at[k, c],
            recv_sem=g_recv.at[far[k], c],
            device_id=(me, partner),
            device_id_type=MESH,
        )

    def recv_wait(source, c):
        pltpu.make_async_remote_copy(
            src_ref=gathered.at[source, pl.ds(c * group, group)],
            dst_ref=gathered.at[source, pl.ds(c * group, group)],
            send_sem=near_send.at[c],
            recv_sem=g_recv.at[source, c],
            device_id=(me, partner),
            device_id_type=MESH,
        ).wait_recv()

    def relay(c):
        for k in range(len(far)):
            recv_wait(far[k], c)
            relay_copy(k, c).start()

    for b in range(blocks):
        ids = []
        for s in range(sel):
            named = chosen_smem[b, s]
            place = named - me * blocks
            ids.append(
                jnp.where(
                    named < 0,
                    null_id,
                    jnp.where(place >= 0, n_kv + place, lax.div(jnp.maximum(named, 0), blocks)),
                )
            )
        keys = [k_pool[n_kv + b] + causal] + [k_pool[i] for i in ids[1:]]
        values = [v_pool[n_kv + b]] + [v_pool[i] for i in ids[1:]]
        scores = lax.dot_general(
            q_stack[b],
            jnp.concatenate(keys, axis=0),
            (((1,), (1,)), ((), ())),
            preferred_element_type=F32,
        )
        peak = jnp.max(scores, axis=1, keepdims=True)
        weights = jnp.exp2(scores - peak).astype(BF16)
        mixed = jnp.dot(weights, jnp.concatenate(values, axis=0), preferred_element_type=F32)
        rolled = pltpu.roll(mixed, HD, 1)
        for t in range(heads // 2):
            even = slice(2 * t * BLK, (2 * t + 1) * BLK)
            odd = slice((2 * t + 1) * BLK, (2 * t + 2) * BLK)
            top = jnp.where(low, rolled[even, :], mixed[odd, :])
            bottom = jnp.where(low, mixed[even, :], rolled[odd, :])
            gathered[tp, b, :, t * 2 * HD : (t + 1) * 2 * HD] = (top / bottom).astype(BF16)
        if (b + 1) % group == 0:
            for k in range(len(far)):
                far_copy(k, b // group).start()
            near_copy(b // group).start()

    loads[7 + parts].wait()
    loads[8 + parts].wait()

    def add_source(source, first, count, fresh):
        height = count * BLK
        view = pl.ds(first * BLK, height)
        heads_f = gathered[source, pl.ds(first, count)].reshape(height, feat).astype(F32)
        squared = heads_f * heads_f
        folded = squared[:, : 2 * HD]
        for t in range(1, feat // (2 * HD)):
            folded = folded + squared[:, t * 2 * HD : (t + 1) * 2 * HD]
        start = pl.multiple_of(source * feat, 2 * HD)
        scaled = (heads_f * gain_ref[:, pl.ds(start, feat)]).astype(BF16)
        product = jnp.dot(scaled, wo[pl.ds(start, feat), :], preferred_element_type=F32)
        if fresh:
            sq_acc[view, :] = folded
            acc[view, :] = product
        else:
            sq_acc[view, :] += folded
            acc[view, :] += product

    def finish(c):
        view = pl.ds(c * group * BLK, group * BLK)
        for k in range(len(far)):
            mate = far[k] + 1 - 2 * lax.rem(far[k], 2)
            recv_wait(mate, c)
            add_source(mate, c * group, group, False)
        inverse = lax.rsqrt(
            jnp.sum(sq_acc[view, :], axis=1, keepdims=True) / total_feat + NORM_EPS
        )
        out_ref[view, :] = (acc[view, :] * inverse).astype(BF16)

    add_source(tp, 0, blocks, True)
    early = 1
    for c in range(early):
        relay(c)
    for c in range(chunks):
        recv_wait(partner, c)
    add_source(partner, 0, blocks, False)
    lag = 1
    for c in range(chunks + lag):
        if c < chunks:
            if c >= early:
                relay(c)
            for k in range(len(far)):
                add_source(far[k], c * group, group, False)
        if c >= lag:
            finish(c - lag)

    def drain(peer):
        @pl.when(peer < me)
        def _():
            ask_copy(me, peer).wait_send()

        @pl.when(peer > me)
        def _():
            kv_copy(me, peer).wait_send()

    peer_loop(drain)
    for c in range(chunks):
        near_copy(c).wait_send()
        for k in range(len(far)):
            far_copy(k, c).wait_send()
            relay_copy(k, c).wait_send()


def per_device(n_kv, n_tp, tokens, w_query, w_key, w_value, w_out, out_gain, chosen):
    rows, width = tokens.shape
    blocks = rows // BLK
    feat = w_query.shape[1]
    out_cols = w_out.shape[1]
    pool = n_kv + blocks + 1
    block_table = np.stack(angle_tables(n_kv * blocks, BLK))
    row_table = np.stack(angle_tables(BLK, 1))
    far = max(n_tp // 2 - 1, 1)
    hbm = pl.BlockSpec(memory_space=pl.ANY)
    vmem = pl.BlockSpec(memory_space=pltpu.VMEM)
    picks = chosen.reshape(blocks, chosen.shape[2])
    dma = pltpu.SemaphoreType.DMA
    return pl.pallas_call(
        functools.partial(kernel, n_kv, n_tp),
        out_shape=pltpu.VMEM((rows, out_cols), BF16),
        in_specs=[hbm] * 9,
        out_specs=vmem,
        scratch_shapes=[
            pltpu.VMEM((1, out_gain.shape[0]), F32),
            pltpu.SMEM(picks.shape, jnp.int32),
            pltpu.VMEM(picks.shape, jnp.int32),
            pltpu.VMEM((2, blocks, 2 * HD), F32),
            pltpu.VMEM((2, BLK, 2 * HD), F32),
            pltpu.VMEM(tokens.shape, BF16),
            pltpu.VMEM(w_query.shape, BF16),
            pltpu.VMEM((2 * HD, width), BF16),
            pltpu.VMEM(w_out.shape, BF16),
            pltpu.VMEM((rows, 2 * HD), F32),
            pltpu.VMEM((rows, 2 * HD), F32),
            pltpu.VMEM((blocks, 2 * HD), jnp.int32),
            pltpu.VMEM((n_kv, blocks, 2 * HD), jnp.int32),
            pltpu.VMEM((blocks, BLK, 2 * HD), BF16),
            pltpu.VMEM((n_kv, BLK, 2 * HD), BF16),
            pltpu.VMEM((n_kv, BLK, 2 * HD), BF16),
            pltpu.VMEM((pool, BLK, 2 * HD), BF16),
            pltpu.VMEM((pool, BLK, 2 * HD), BF16),
            pltpu.VMEM((blocks, feat // HD * BLK, 2 * HD), BF16),
            pltpu.VMEM((n_tp, blocks, BLK, feat), BF16),
            pltpu.VMEM((rows, out_cols), F32),
            pltpu.VMEM((rows, 2 * HD), F32),
            dma((11,)),
            dma((n_kv,)),
            dma((n_kv,)),
            dma((n_kv,)),
            dma((n_kv,)),
            dma((blocks,)),
            dma((far, blocks)),
            dma((far, blocks)),
            dma((n_tp, blocks)),
        ],
        compiler_params=pltpu.CompilerParams(collective_id=0, has_side_effects=True),
        name="layer",
    )(
        tokens,
        w_query,
        w_key.T,
        w_value.T,
        w_out,
        out_gain.reshape(1, -1),
        picks,
        block_table,
        row_table,
    )


def solution(mesh):
    return jax.shard_map(
        functools.partial(per_device, mesh.shape["kv"], mesh.shape["tp"]),
        mesh=mesh,
        in_specs=(
            P("kv", None),
            P(None, "tp"),
            P(None, "tp"),
            P(None, "tp"),
            P(None, "tp"),
            P(),
            P("tp", "kv", None),
        ),
        out_specs=P("kv", "tp"),
        check_vma=False,
    )
```
